32 devices in a mesh: sp: 4 (over y, core), dp: 8 (over z, x).
Axes of the slice: x: 2, y: 2, z: 4, core: 2. Of those that a mesh axis runs over, the one named last changes fastest.
Arguments:
- stream: bfloat16 [8, 512, 2064], P('dp', 'sp'), may hold values from -6 to 6
- mix_gain: float32 [2064], replicated, may hold values from 0.1 to 1.9
- query_weight: bfloat16 [2064, 2048], P('dp'), may hold values from -0.125 to 0.125
- query_gain: float32 [128], replicated, may hold values from 0.1 to 1.9
- keys: bfloat16 [8, 512, 512], P('dp', 'sp'), may hold values from -6 to 6
- key_gain: float32 [128], replicated, may hold values from 0.1 to 1.9
- values: bfloat16 [8, 512, 512], P('dp', 'sp'), may hold values from -48 to 48
- stick_offset: float32 [16], replicated, may hold values from -8.5 to -7, as said below
Outputs:
- attended: bfloat16 [8, 512, 2048], P('dp', 'sp')
The draws below stay inside these ranges and needn't reach their ends.
Inputs may be any that keep to these rules, and one draw needn't show every extreme that they name: `stick_offset`: one offset for each query head, added to all of that head's scores.
All inputs are finite; a program needn't handle non-finite values.
Results may differ from the reference program's by a relative error of at most 0.012.
Values may be sent and summed in bfloat16 or wider, within the bound.
A program may use at most 64 MiB of HBM per device.

```python
import math
import jax
import jax.numpy as jnp
from jax import lax

D = 2064
QUERY_HEADS = 16
KV_HEADS = 4
HEAD_DIM = 128
LENGTH = 512
SEQS = 8


def draw_stick_offset(key, part):
    base = jax.random.fold_in(key, 7)
    first_key, second_key = jax.random.split(base, 2)
    return jax.random.uniform(second_key, (QUERY_HEADS,), jnp.float32, -8.5, -7.0)


def level_of(rng, extent, shards, low, largest):
    level, own = 1.0, jax.random.fold_in(rng, 6)
    for position, shards_of in shards:
        heights = jnp.exp(jax.random.uniform(jax.random.fold_in(own, position), (shards_of,), jnp.float32, low / len(shards), largest / len(shards)))
        level = level * jnp.repeat(heights, extent[position] // shards_of).reshape([-1 if axis == position else 1 for axis in range(len(extent))])
    return level


def bell_draw(own_key, dims, deviation, most, pieces=(), kind=jnp.bfloat16):
    level = level_of(own_key, dims, pieces, -0.22, 0.18) if pieces else 1.0
    entries = jax.random.normal(own_key, dims, jnp.float32) * deviation * level
    return jnp.minimum(jnp.maximum(entries, -most), most).astype(kind)


def setup_inputs(seed: int = 0) -> dict:
    key_of = jax.random.split(jax.random.key(seed), 9)
    return {
        "stream": bell_draw(key_of[0], (SEQS, LENGTH, D), 1.0, 6.0, ((0, 8), (1, 4))),
        "mix_gain": jnp.clip(1.0 + 0.18 * jax.random.normal(key_of[1], (D,), jnp.float32), 0.1, 1.9),
        "query_weight": bell_draw(key_of[2], (D, QUERY_HEADS * HEAD_DIM), D ** -0.5, 0.125, ((0, 8),)),
        "query_gain": jnp.clip(1.0 + 0.18 * jax.random.normal(key_of[3], (HEAD_DIM,), jnp.float32), 0.1, 1.9),
        "keys": bell_draw(key_of[4], (SEQS, LENGTH, KV_HEADS * HEAD_DIM), 1.0, 6.0, ((0, 8), (1, 4))),
        "key_gain": jnp.clip(1.0 + 0.18 * jax.random.normal(key_of[5], (HEAD_DIM,), jnp.float32), 0.1, 1.9),
        "values": bell_draw(key_of[6], (SEQS, LENGTH, KV_HEADS * HEAD_DIM), 8.0, 48.0, ((0, 8), (1, 4))),
        "stick_offset": draw_stick_offset(jax.random.fold_in(key_of[8], 71), 0),
    }


norm_eps = 1e-06
row_block = 512

def rms_scaled(inputs, gain):
    wide = inputs.astype(jnp.float32)
    scaled = wide * lax.rsqrt(lax.optimization_barrier(jnp.mean(wide * wide, axis=-1, keepdims=True)) + norm_eps) * gain
    return scaled.astype(jnp.bfloat16)

def stick_weights(scores, first_row):
    rows_here = scores.shape[-2]
    keys_here = scores.shape[-1]
    query_pos = first_row + jnp.arange(rows_here, dtype=jnp.int32)
    key_pos = jnp.arange(keys_here, dtype=jnp.int32)
    causal = key_pos[None, :] < query_pos[:, None]
    log_keep = jnp.where(causal, jax.nn.log_sigmoid(-scores), 0.0)
    tail = lax.cumsum(log_keep, axis=scores.ndim - 1, reverse=True) - log_keep
    return jnp.where(causal, jnp.exp(jax.nn.log_sigmoid(scores) + tail), 0.0)

def head_output(query_rows, key_rows, value_rows, offset):
    seq_length = query_rows.shape[0]
    block = math.gcd(seq_length, row_block)
    outputs = []
    for block_id in range(seq_length // block):
        first = block_id * block
        finish = first + block
        scores = jnp.dot(query_rows[first:finish], key_rows[:finish].T, preferred_element_type=jnp.float32)
        scores = scores * HEAD_DIM ** (-0.5) + offset
        weights = stick_weights(scores, first).astype(jnp.bfloat16)
        outputs.append(jnp.dot(weights, value_rows[:finish], preferred_element_type=jnp.float32))
    return jnp.concatenate(outputs, axis=0).astype(jnp.bfloat16)

def reference(stream, mix_gain, query_weight, query_gain, keys, key_gain, values, stick_offset):
    group_size = QUERY_HEADS // KV_HEADS

    def one_sequence(inputs):
        stream_rows, key_rows, value_rows = inputs
        normed = rms_scaled(stream_rows, mix_gain)
        queries = jnp.dot(normed, query_weight, preferred_element_type=jnp.float32).astype(jnp.bfloat16)
        queries = lax.optimization_barrier(queries)
        query_heads = rms_scaled(queries.reshape(LENGTH, QUERY_HEADS, HEAD_DIM), query_gain)
        key_heads = rms_scaled(key_rows.reshape(LENGTH, KV_HEADS, HEAD_DIM), key_gain)
        value_heads = value_rows.reshape(LENGTH, KV_HEADS, HEAD_DIM)

        def one_head(head_id):
            kv_id = head_id // group_size
            query_one = lax.dynamic_index_in_dim(query_heads, head_id, 1, keepdims=False)
            key_one = lax.dynamic_index_in_dim(key_heads, kv_id, 1, keepdims=False)
            value_one = lax.dynamic_index_in_dim(value_heads, kv_id, 1, keepdims=False)
            return head_output(query_one, key_one, value_one, stick_offset[head_id])
        outputs = lax.map(one_head, jnp.arange(QUERY_HEADS, dtype=jnp.int32))
        return outputs.transpose(1, 0, 2).reshape(LENGTH, QUERY_HEADS * HEAD_DIM)
    return lax.map(one_sequence, (stream, keys, values))
```

```python
import functools
import math

import jax
import jax.numpy as jnp
from jax import lax
from jax.experimental import pallas as pl
from jax.experimental.pallas import tpu as pltpu
from jax.sharding import PartitionSpec as P

norm_eps = 1e-06
row_block = 256
key_block = 128
MESH = pl.DeviceIdType.MESH


def rms_scaled(inputs, gain):
    wide = inputs.astype(jnp.float32)
    scaled = wide * lax.rsqrt(jnp.mean(wide * wide, axis=-1, keepdims=True) + norm_eps) * gain
    return scaled.astype(jnp.bfloat16)


def stick_weights(scores, first_row):
    heads_here = scores.shape[0]
    rows_here = scores.shape[1]
    keys_here = scores.shape[2]
    width = math.gcd(keys_here, key_block)
    blocks_here = keys_here // width
    query_pos = first_row + jnp.arange(rows_here, dtype=jnp.int32)
    key_pos = jnp.arange(keys_here, dtype=jnp.int32)
    causal = key_pos[None, :] < query_pos[:, None]
    log_keep = jnp.where(causal, jax.nn.log_sigmoid(-scores), 0.0)
    pieces = log_keep.reshape(heads_here, rows_here, blocks_here, width)
    inner = jnp.arange(width, dtype=jnp.int32)
    upper = (inner[:, None] > inner[None, :]).astype(jnp.float32)
    local = jnp.einsum("hqbk,kj->hqbj", pieces, upper, precision=lax.Precision.HIGHEST)
    totals = jnp.sum(pieces, axis=3)
    later = lax.cumsum(totals, axis=2, reverse=True) - totals
    tail = (local + later[:, :, :, None]).reshape(heads_here, rows_here, keys_here)
    return jnp.where(causal, jnp.exp(jax.nn.log_sigmoid(scores) + tail), 0.0)


def general_body(stream, mix_gain, query_weight, query_gain, keys, key_gain, values, stick_offset):
    sp_count = lax.axis_size("sp")
    sp_index = lax.axis_index("sp")
    stream_rows = stream[0]
    tokens_dev = stream_rows.shape[0]
    head_width = query_gain.shape[0]
    heads_all = stick_offset.shape[0]
    heads_dev = heads_all // sp_count
    kv_count = keys.shape[2] // head_width
    group_size = sp_count // kv_count
    seq_length = tokens_dev * sp_count
    stacked = jnp.stack((keys[0], values[0]), axis=1).reshape(tokens_dev, 2, kv_count, head_width)
    copied = jnp.repeat(stacked, group_size, axis=2)
    arrived = lax.all_to_all(copied, "sp", split_axis=2, concat_axis=0, tiled=True)
    key_value = arrived[:, :, 0, :]
    normed = rms_scaled(stream_rows, mix_gain)
    columns = lax.dynamic_slice_in_dim(
        query_weight, sp_index * (heads_dev * head_width), heads_dev * head_width, 1
    )
    gathered = lax.all_gather(columns, "dp", axis=0, tiled=True)
    queries = jnp.dot(
        lax.all_gather(normed, "sp", axis=0, tiled=True),
        gathered,
        preferred_element_type=jnp.float32,
    ).astype(jnp.bfloat16)
    queries = lax.optimization_barrier(queries)
    mine = rms_scaled(queries.reshape(seq_length, heads_dev, head_width), query_gain)
    key_heads = rms_scaled(key_value[:, 0], key_gain)
    value_rows = key_value[:, 1]
    offsets = lax.dynamic_slice_in_dim(stick_offset, sp_index * heads_dev, heads_dev)
    block = math.gcd(seq_length, row_block)
    outputs = []
    for block_id in range(seq_length // block):
        first = block_id * block
        finish = first + block
        scores = jnp.einsum(
            "qhd,kd->hqk",
            mine[first:finish],
            key_heads[:finish],
            preferred_element_type=jnp.float32,
        )
        scores = scores * head_width ** (-0.5) + offsets[:, None, None]
        weights = stick_weights(scores, first).astype(jnp.bfloat16)
        outputs.append(
            jnp.einsum(
                "hqk,kd->qhd", weights, value_rows[:finish], preferred_element_type=jnp.float32
            )
        )
    attended = (
        jnp.concatenate(outputs, axis=0)
        .reshape(seq_length, heads_dev * head_width)
        .astype(jnp.bfloat16)
    )
    returned = lax.all_to_all(attended, "sp", split_axis=0, concat_axis=1, tiled=True)
    return returned[None]


def kernel(
    nz, nx, heads, stream, mix_gain, weight, query_gain, keys, key_gain, values, offset, out,
    xraw, xs, wb, kraw, kn, vb, acc, ob,
    own_sem, wrecv, wsend, xrecv, xsend, krecv, ksend, vrecv, vsend, orecv, osend,
):
    sp_count = xraw.shape[0]
    tokens, width = xraw.shape[1:]
    seq = sp_count * tokens
    hd = query_gain.shape[1]
    depth = wb.shape[1]
    dp_count = nz * nx
    dp = lax.axis_index("dp")
    sp = lax.axis_index("sp")
    z, x = dp // nx, lax.rem(dp, nx)
    side = z * nx + (1 - x)
    pair = 2 * (sp // 2) + (1 - lax.rem(sp, 2))
    across = lax.rem(sp + 2, sp_count)
    corner = lax.rem(pair + 2, sp_count)
    peers = (across, pair, corner)
    chunks = xrecv.shape[1]
    part = tokens // chunks

    barrier = pltpu.get_barrier_semaphore()
    for peer in peers:
        pl.semaphore_signal(barrier, inc=1, device_id={"sp": peer}, device_id_type=MESH)
    pl.semaphore_signal(barrier, inc=1, device_id={"dp": side}, device_id_type=MESH)
    has_up, has_down = z < nz - 1, z > 0

    @pl.when(has_up)
    def _():
        pl.semaphore_signal(barrier, inc=1, device_id={"dp": dp + nx}, device_id_type=MESH)

    @pl.when(has_down)
    def _():
        pl.semaphore_signal(barrier, inc=1, device_id={"dp": dp - nx}, device_id_type=MESH)

    pl.semaphore_wait(barrier, 4 + jnp.where(has_up, 1, 0) + jnp.where(has_down, 1, 0))

    base = sp * (heads * hd)
    low, high = z, nz - 1 - z
    both = jnp.minimum(low, high)

    def order(i):
        if i == 0:
            return z
        near = z + (i + 1) // 2 if i % 2 else z - i // 2
        far = jnp.where(high > low, z + (i - both), z - (i - both))
        return jnp.where(i <= 2 * both, near, far)

    def w_copy(link, target, rank, h):
        zz = order(rank)
        block = zz * nx + x
        if rank == 0:
            src = weight.at[:, pl.ds(pl.multiple_of(base + h * hd, hd), hd)]
        else:
            src = wb.at[block, :, pl.ds(h * hd, hd)]
        return pltpu.make_async_remote_copy(
            src_ref=src,
            dst_ref=wb.at[block, :, pl.ds(h * hd, hd)],
            send_sem=wsend.at[link, rank, h],
            recv_sem=wrecv.at[block, h],
            device_id={"dp": target},
            device_id_type=MESH,
        )

    def w_send(rank, h, act):
        zz = order(rank)

        @pl.when(has_up & (zz <= z))
        def _():
            act(w_copy(0, dp + nx, rank, h))

        @pl.when(has_down & (zz >= z))
        def _():
            act(w_copy(1, dp - nx, rank, h))

        act(w_copy(2, side, rank, h))

    def w_wait(block, h):
        ref = wb.at[block, :, pl.ds(h * hd, hd)]
        pltpu.make_async_remote_copy(
            src_ref=ref, dst_ref=ref, send_sem=wsend.at[0, 0, 0], recv_sem=wrecv.at[block, h],
            device_id={"dp": side}, device_id_type=MESH,
        ).wait_recv()

    def start(copy):
        copy.start()

    def finish_send(copy):
        copy.wait_send()

    def x_copy(source, c, link, target):
        rows = pl.ds(c * part, part)
        src = stream.at[0, rows] if link < 2 else xraw.at[source, rows]
        return pltpu.make_async_remote_copy(
            src_ref=src, dst_ref=xraw.at[source, rows],
            send_sem=xsend.at[link, c], recv_sem=xrecv.at[source, c],
            device_id={"sp": target}, device_id_type=MESH,
        )

    def kv_copy(which, p):
        hbm, buf, ssem, rsem = ((keys, kraw, ksend, krecv), (values, vb, vsend, vrecv))[which]
        peer = peers[p]
        return pltpu.make_async_remote_copy(
            src_ref=hbm.at[0, :, pl.ds(pl.multiple_of(peer * hd, hd), hd)],
            dst_ref=buf.at[pl.ds(pl.multiple_of(sp * tokens, tokens), tokens)],
            send_sem=ssem.at[p], recv_sem=rsem.at[sp],
            device_id={"sp": peer}, device_id_type=MESH,
        )

    for h in range(heads):
        w_send(0, h, start)
        if h == 0:
            for c in range(chunks):
                x_copy(sp, c, 0, across).start()
                x_copy(sp, c, 1, pair).start()
    own_x = pltpu.make_async_copy(stream.at[0], xraw.at[sp], own_sem.at[0])
    own_x.start()
    own_w = pltpu.make_async_copy(
        weight.at[:, pl.ds(pl.multiple_of(base, hd), heads * hd)], wb.at[dp], own_sem.at[1]
    )
    own_w.start()
    here = pl.ds(pl.multiple_of(sp * tokens, tokens), tokens)
    mine = pl.ds(pl.multiple_of(sp * hd, hd), hd)
    own_k = pltpu.make_async_copy(keys.at[0, :, mine], kraw.at[here], own_sem.at[2])
    own_v = pltpu.make_async_copy(values.at[0, :, mine], vb.at[here], own_sem.at[3])
    own_k.start()
    own_v.start()
    for p in range(3):
        kv_copy(0, p).start()
        kv_copy(1, p).start()

    def norm_rows(source, c):
        step = 32

        def inner(i, carry):
            at = pl.multiple_of(c * part + i * step, step)
            wide = xraw[source, pl.ds(at, step), :].astype(jnp.float32)
            scale = lax.rsqrt(jnp.mean(wide * wide, axis=-1, keepdims=True) + norm_eps)
            done = (wide * scale * mix_gain[...]).astype(jnp.bfloat16)
            to = pl.ds(pl.multiple_of(source * tokens + at, step), step)
            for d in range(dp_count):
                xs[d, to, :] = done[:, d * depth : (d + 1) * depth]
            return carry

        lax.fori_loop(0, part // step, inner, 0)

    def accumulate(block, first=False):
        tile = 256
        for n in range(0, heads * hd, tile):
            term = jnp.dot(xs[block], wb[block, :, n : n + tile], preferred_element_type=jnp.float32)
            if first:
                acc[:, n : n + tile] = term
            else:
                acc[:, n : n + tile] += term

    own_x.wait()
    for c in range(chunks):
        norm_rows(sp, c)
    for h in range(heads):
        w_wait(order(1) * nx + x, h)
        w_send(1, h, start)
    for c in range(chunks):
        x_copy(pair, c, 1, pair).wait_recv()
        norm_rows(pair, c)
    for rank in range(2, nz - 1):
        for h in range(heads):
            w_wait(order(rank) * nx + x, h)
            w_send(rank, h, start)
    for c in range(chunks):
        x_copy(across, c, 0, across).wait_recv()
        x_copy(across, c, 2, pair).start()
    for c in range(chunks):
        norm_rows(across, c)

    own_k.wait()
    own_v.wait()
    for p in range(3):
        rows = pl.ds(pl.multiple_of(peers[p] * tokens, tokens), tokens)
        for buf, rsem, ssem in ((kraw, krecv, ksend), (vb, vrecv, vsend)):
            pltpu.make_async_remote_copy(
                src_ref=buf.at[rows], dst_ref=buf.at[rows], send_sem=ssem.at[p],
                recv_sem=rsem.at[peers[p]], device_id={"sp": peers[p]}, device_id_type=MESH,
            ).wait_recv()
    kn[...] = rms_scaled(kraw[...], key_gain[...])

    for c in range(chunks):
        x_copy(corner, c, 2, pair).wait_recv()
        norm_rows(corner, c)

    own_w.wait()
    accumulate(dp, True)
    for rank in range(1, nz - 1):
        accumulate(order(rank) * nx + x)
    for h in range(heads):
        w_wait(order(nz - 1) * nx + x, h)
        w_send(nz - 1, h, start)
    accumulate(order(nz - 1) * nx + x)
    for rank in range(nz - 1):
        block = order(rank) * nx + (1 - x)
        for h in range(heads):
            w_wait(block, h)
        accumulate(block)

    last = order(nz - 1) * nx + (1 - x)
    size = math.gcd(seq, row_block)
    rowi = lax.broadcasted_iota(jnp.int32, (size, size), 0)
    coli = lax.broadcasted_iota(jnp.int32, (size, size), 1)
    causal = coli < rowi
    suffix = (rowi >= coli).astype(jnp.float32).astype(jnp.bfloat16)

    def o_copy(h, p, incoming=False):
        peer = peers[p]
        owner = peer if incoming else sp
        return pltpu.make_async_remote_copy(
            src_ref=ob.at[h, pl.ds(pl.multiple_of(peer * tokens, tokens), tokens)],
            dst_ref=out.at[0, :, pl.ds(pl.multiple_of(owner * (heads * hd) + h * hd, hd), hd)],
            send_sem=osend.at[p, h], recv_sem=orecv.at[owner, h],
            device_id={"sp": peer}, device_id_type=MESH,
        )

    def o_local(h):
        return pltpu.make_async_copy(
            ob.at[h, here],
            out.at[0, :, pl.ds(pl.multiple_of(base + h * hd, hd), hd)],
            own_sem.at[4 + h],
        )

    for h in range(heads):
        w_wait(last, h)
        cols = slice(h * hd, (h + 1) * hd)
        total = acc[:, cols] + jnp.dot(
            xs[last], wb[last, :, cols], preferred_element_type=jnp.float32
        )
        qn = rms_scaled(total.astype(jnp.bfloat16), query_gain[...])
        off = offset[sp * heads + h]
        for rb in range(seq // size):
            q = qn[rb * size : (rb + 1) * size]
            carry, result = None, None
            for kb in reversed(range(rb + 1)):
                at = slice(kb * size, (kb + 1) * size)
                s = lax.dot_general(
                    q, kn[at], (((1,), (1,)), ((), ())), preferred_element_type=jnp.float32
                )
                s = s * hd ** (-0.5) + off
                soft = jnp.log(1.0 + jnp.exp(s))
                if kb == rb:
                    soft = jnp.where(causal, soft, 0.0)
                upper = soft.astype(jnp.bfloat16)
                lower = (soft - upper.astype(jnp.float32)).astype(jnp.bfloat16)
                sums = jnp.dot(upper, suffix, preferred_element_type=jnp.float32) + jnp.dot(
                    lower, suffix, preferred_element_type=jnp.float32
                )
                if carry is not None:
                    sums = sums + carry
                carry = sums[:, 0:1]
                w = jnp.exp(s - sums)
                if kb == rb:
                    w = jnp.where(causal, w, 0.0)
                term = jnp.dot(w.astype(jnp.bfloat16), vb[at], preferred_element_type=jnp.float32)
                result = term if result is None else result + term
            ob[h, rb * size : (rb + 1) * size, :] = result.astype(jnp.bfloat16)
        for p in (0, 2, 1):
            o_copy(h, p).start()
        o_local(h).start()

    for rank in range(nz):
        for h in range(heads):
            w_send(rank, h, finish_send)
    for c in range(chunks):
        x_copy(sp, c, 0, across).wait_send()
        x_copy(sp, c, 1, pair).wait_send()
        x_copy(across, c, 2, pair).wait_send()
    for p in range(3):
        kv_copy(0, p).wait_send()
        kv_copy(1, p).wait_send()
    for h in range(heads):
        o_local(h).wait()
        for p in range(3):
            o_copy(h, p).wait_send()
            o_copy(h, p, True).wait_recv()


def fused_body(nx, stream, mix_gain, query_weight, query_gain, keys, key_gain, values, stick_offset):
    sp_count = lax.axis_size("sp")
    dp_count = lax.axis_size("dp")
    nz = dp_count // nx
    tokens, width = stream.shape[1:]
    depth, columns = query_weight.shape
    hd = query_gain.shape[0]
    heads = stick_offset.shape[0] // sp_count
    seq = tokens * sp_count
    chunks = 2
    vmem = pl.BlockSpec(memory_space=pltpu.VMEM)
    hbm = pl.BlockSpec(memory_space=pl.ANY)
    dma = pltpu.SemaphoreType.DMA
    return pl.pallas_call(
        functools.partial(kernel, nz, nx, heads),
        out_shape=jax.ShapeDtypeStruct((1, tokens, columns), jnp.bfloat16),
        in_specs=[hbm, vmem, hbm, vmem, hbm, vmem, hbm, pl.BlockSpec(memory_space=pltpu.SMEM)],
        out_specs=hbm,
        scratch_shapes=[
            pltpu.VMEM((sp_count, tokens, width), jnp.bfloat16),
            pltpu.VMEM((dp_count, seq, depth), jnp.bfloat16),
            pltpu.VMEM((dp_count, depth, heads * hd), jnp.bfloat16),
            pltpu.VMEM((seq, hd), jnp.bfloat16),
            pltpu.VMEM((seq, hd), jnp.bfloat16),
            pltpu.VMEM((seq, hd), jnp.bfloat16),
            pltpu.VMEM((seq, heads * hd), jnp.float32),
            pltpu.VMEM((heads, seq, hd), jnp.bfloat16),
            dma((4 + heads,)),
            dma((dp_count, heads)),
            dma((3, nz, heads)),
            dma((sp_count, chunks)),
            dma((3, chunks)),
            dma((sp_count,)),
            dma((3,)),
            dma((sp_count,)),
            dma((3,)),
            dma((sp_count, heads)),
            dma((3, heads)),
        ],
        compiler_params=pltpu.CompilerParams(
            collective_id=0, has_side_effects=True, vmem_limit_bytes=48 * 1024 * 1024
        ),
    )(
        stream, mix_gain[None], query_weight, query_gain[None], keys, key_gain[None], values,
        stick_offset,
    )


def widths(mesh):
    names = tuple(mesh.axis_names)
    grid = mesh.devices if names == ("dp", "sp") else mesh.devices.T
    nx = len({d.coords[0] for d in grid[:, 0]})
    ny = len({d.coords[1] for d in grid[0]})
    return nx, ny


def solution(mesh):
    nx, ny = widths(mesh)
    pairs = nx == 2 and ny == 2

    def body(*args):
        stream, _, _, query_gain, keys = args[:5]
        sp_count = lax.axis_size("sp")
        one_head = keys.shape[2] // query_gain.shape[0] == sp_count
        if pairs and one_head and sp_count == 2 * ny:
            return fused_body(nx, *args)
        return general_body(*args)

    return jax.shard_map(
        body,
        mesh=mesh,
        in_specs=(
            P("dp", "sp", None),
            P(),
            P("dp", None),
            P(),
            P("dp", "sp", None),
            P(),
            P("dp", "sp", None),
            P(),
        ),
        out_specs=P("dp", "sp", None),
        check_vma=False,
    )
```

```python
import functools
import math

import jax
import jax.numpy as jnp
from jax import lax
from jax.experimental import pallas as pl
from jax.experimental.pallas import tpu as pltpu
from jax.sharding import PartitionSpec as P

norm_eps = 1e-06
row_block = 256
key_block = 128
MESH = pl.DeviceIdType.MESH


def rms_scaled(inputs, gain):
    wide = inputs.astype(jnp.float32)
    scaled = wide * lax.rsqrt(jnp.mean(wide * wide, axis=-1, keepdims=True) + norm_eps) * gain
    return scaled.astype(jnp.bfloat16)


def stick_weights(scores, first_row):
    heads_here = scores.shape[0]
    rows_here = scores.shape[1]
    keys_here = scores.shape[2]
    width = math.gcd(keys_here, key_block)
    blocks_here = keys_here // width
    query_pos = first_row + jnp.arange(rows_here, dtype=jnp.int32)
    key_pos = jnp.arange(keys_here, dtype=jnp.int32)
    causal = key_pos[None, :] < query_pos[:, None]
    log_keep = jnp.where(causal, jax.nn.log_sigmoid(-scores), 0.0)
    pieces = log_keep.reshape(heads_here, rows_here, blocks_here, width)
    inner = jnp.arange(width, dtype=jnp.int32)
    upper = (inner[:, None] > inner[None, :]).astype(jnp.float32)
    local = jnp.einsum("hqbk,kj->hqbj", pieces, upper, precision=lax.Precision.HIGHEST)
    totals = jnp.sum(pieces, axis=3)
    later = lax.cumsum(totals, axis=2, reverse=True) - totals
    tail = (local + later[:, :, :, None]).reshape(heads_here, rows_here, keys_here)
    return jnp.where(causal, jnp.exp(jax.nn.log_sigmoid(scores) + tail), 0.0)


def general_body(stream, mix_gain, query_weight, query_gain, keys, key_gain, values, stick_offset):
    sp_count = lax.axis_size("sp")
    sp_index = lax.axis_index("sp")
    stream_rows = stream[0]
    tokens_dev = stream_rows.shape[0]
    head_width = query_gain.shape[0]
    heads_all = stick_offset.shape[0]
    heads_dev = heads_all // sp_count
    kv_count = keys.shape[2] // head_width
    group_size = sp_count // kv_count
    seq_length = tokens_dev * sp_count
    stacked = jnp.stack((keys[0], values[0]), axis=1).reshape(tokens_dev, 2, kv_count, head_width)
    copied = jnp.repeat(stacked, group_size, axis=2)
    arrived = lax.all_to_all(copied, "sp", split_axis=2, concat_axis=0, tiled=True)
    key_value = arrived[:, :, 0, :]
    normed = rms_scaled(stream_rows, mix_gain)
    columns = lax.dynamic_slice_in_dim(
        query_weight, sp_index * (heads_dev * head_width), heads_dev * head_width, 1
    )
    gathered = lax.all_gather(columns, "dp", axis=0, tiled=True)
    queries = jnp.dot(
        lax.all_gather(normed, "sp", axis=0, tiled=True),
        gathered,
        preferred_element_type=jnp.float32,
    ).astype(jnp.bfloat16)
    queries = lax.optimization_barrier(queries)
    mine = rms_scaled(queries.reshape(seq_length, heads_dev, head_width), query_gain)
    key_heads = rms_scaled(key_value[:, 0], key_gain)
    value_rows = key_value[:, 1]
    offsets = lax.dynamic_slice_in_dim(stick_offset, sp_index * heads_dev, heads_dev)
    block = math.gcd(seq_length, row_block)
    outputs = []
    for block_id in range(seq_length // block):
        first = block_id * block
        finish = first + block
        scores = jnp.einsum(
            "qhd,kd->hqk",
            mine[first:finish],
            key_heads[:finish],
            preferred_element_type=jnp.float32,
        )
        scores = scores * head_width ** (-0.5) + offsets[:, None, None]
        weights = stick_weights(scores, first).astype(jnp.bfloat16)
        outputs.append(
            jnp.einsum(
                "hqk,kd->qhd", weights, value_rows[:finish], preferred_element_type=jnp.float32
            )
        )
    attended = (
        jnp.concatenate(outputs, axis=0)
        .reshape(seq_length, heads_dev * head_width)
        .astype(jnp.bfloat16)
    )
    returned = lax.all_to_all(attended, "sp", split_axis=0, concat_axis=1, tiled=True)
    return returned[None]


def kernel(
    nz, nx, heads, stream, mix_gain, weight, query_gain, keys, key_gain, values, offset, out,
    xraw, xs, wb, kraw, kn, vb, acc, ob,
    own_sem, wrecv, zsend, wsend, fsend, xrecv, xsend, krecv, ksend, vrecv, vsend, orecv, osend,
):
    sp_count = xraw.shape[0]
    tokens, width = xraw.shape[1:]
    seq = sp_count * tokens
    hd = query_gain.shape[0]
    depth = wb.shape[1]
    dp_count = nz * nx
    dp = lax.axis_index("dp")
    sp = lax.axis_index("sp")
    z, x = dp // nx, lax.rem(dp, nx)
    side = z * nx + (1 - x)
    pair = 2 * (sp // 2) + (1 - lax.rem(sp, 2))
    across = lax.rem(sp + 2, sp_count)
    corner = lax.rem(pair + 2, sp_count)
    peers = (across, pair, corner)
    chunks = xrecv.shape[1]
    part = tokens // chunks

    barrier = pltpu.get_barrier_semaphore()
    for peer in peers:
        pl.semaphore_signal(barrier, inc=1, device_id={"sp": peer}, device_id_type=MESH)
    pl.semaphore_signal(barrier, inc=1, device_id={"dp": side}, device_id_type=MESH)
    has_up, has_down = z < nz - 1, z > 0

    @pl.when(has_up)
    def _():
        pl.semaphore_signal(barrier, inc=1, device_id={"dp": dp + nx}, device_id_type=MESH)

    @pl.when(has_down)
    def _():
        pl.semaphore_signal(barrier, inc=1, device_id={"dp": dp - nx}, device_id_type=MESH)

    pl.semaphore_wait(barrier, 4 + jnp.where(has_up, 1, 0) + jnp.where(has_down, 1, 0))

    base = sp * (heads * hd)
    low, high = z, nz - 1 - z
    both = jnp.minimum(low, high)

    upper_half = low > high

    def order(i):
        if i == 0:
            return z
        step = (i + 1) // 2 if i % 2 else -(i // 2)
        near = jnp.where(upper_half, z + step, z - step)
        far = jnp.where(upper_half, z - (i - both), z + (i - both))
        return jnp.where(i <= 2 * both, near, far)

    def w_copy(block, h, sem, target, own=False):
        ref = wb.at[block, :, pl.ds(h * hd, hd)]
        src = weight.at[:, pl.ds(pl.multiple_of(base + h * hd, hd), hd)] if own else ref
        return pltpu.make_async_remote_copy(
            src_ref=src, dst_ref=ref, send_sem=sem, recv_sem=wrecv.at[block, h],
            device_id={"dp": target}, device_id_type=MESH,
        )

    def z_send(k, h, act):
        @pl.when((z + k < nz) & has_down)
        def _():
            act(w_copy((z + k) * nx + x, h, zsend.at[0, k, h], dp - nx, k == 0))

        @pl.when((z - k >= 0) & has_up)
        def _():
            act(w_copy((z - k) * nx + x, h, zsend.at[1, k, h], dp + nx, k == 0))

    def z_step(k, h):
        @pl.when(z + k < nz)
        def _():
            w_wait((z + k) * nx + x, h)

        @pl.when(z - k >= 0)
        def _():
            w_wait((z - k) * nx + x, h)

        z_send(k, h, start)

    def side_send(rank, h, act):
        if rank < nz - 1 or h % 2 == 0:
            act(w_copy(order(rank) * nx + x, h, wsend.at[rank, h], side, rank == 0))

    inner = both == nz // 2 - 1
    inward = jnp.where(upper_half, dp - nx, dp + nx)
    outward = jnp.where(upper_half, dp + nx, dp - nx)
    edge = jnp.where(upper_half, nz - 1, 0) * nx + (1 - x)
    opposite = jnp.where(upper_half, 0, nz - 1) * nx + (1 - x)

    def far_in(h, act):
        @pl.when(inner)
        def _():
            act(w_copy(edge, h, fsend.at[0, h], inward))

    def far_out(h, act):
        @pl.when(both > 0)
        def _():
            act(w_copy(opposite, h, fsend.at[1, h], outward))

    def far_in_step(h):
        @pl.when(inner)
        def _():
            w_wait(edge, h)

        far_in(h, start)

    def far_out_step(h):
        w_wait(opposite, h)
        far_out(h, start)

    def side_wait(rank, h):
        if rank == nz - 1 and h % 2:
            return
        if rank == nz - 3 and h % 2:

            @pl.when(jnp.logical_not(inner))
            def _():
                w_wait(order(rank) * nx + (1 - x), h)
        else:
            w_wait(order(rank) * nx + (1 - x), h)

    def w_wait(block, h):
        ref = wb.at[block, :, pl.ds(h * hd, hd)]
        pltpu.make_async_remote_copy(
            src_ref=ref, dst_ref=ref, send_sem=wsend.at[0, 0], recv_sem=wrecv.at[block, h],
            device_id={"dp": side}, device_id_type=MESH,
        ).wait_recv()

    def start(copy):
        copy.start()

    def finish_send(copy):
        copy.wait_send()

    def x_copy(source, c, link, target):
        rows = pl.ds(c * part, part)
        src = stream.at[0, rows] if link < 2 else xraw.at[source, rows]
        return pltpu.make_async_remote_copy(
            src_ref=src, dst_ref=xraw.at[source, rows],
            send_sem=xsend.at[link, c], recv_sem=xrecv.at[source, c],
            device_id={"sp": target}, device_id_type=MESH,
        )

    def kv_copy(which, p):
        hbm, buf, ssem, rsem = ((keys, kraw, ksend, krecv), (values, vb, vsend, vrecv))[which]
        peer = peers[p]
        return pltpu.make_async_remote_copy(
            src_ref=hbm.at[0, :, pl.ds(pl.multiple_of(peer * hd, hd), hd)],
            dst_ref=buf.at[pl.ds(pl.multiple_of(sp * tokens, tokens), tokens)],
            send_sem=ssem.at[p], recv_sem=rsem.at[sp],
            device_id={"sp": peer}, device_id_type=MESH,
        )

    def both_send(k, h):
        z_send(k, h, start)
        side_send(k, h, start)

    both_send(0, 0)
    for c in range(chunks):
        x_copy(sp, c, 0, across).start()
        x_copy(sp, c, 1, pair).start()
    for h in range(1, heads - 1):
        both_send(0, h)
    own_x = pltpu.make_async_copy(stream.at[0], xraw.at[sp], own_sem.at[0])
    own_x.start()
    own_w = pltpu.make_async_copy(
        weight.at[:, pl.ds(pl.multiple_of(base, hd), heads * hd)], wb.at[dp], own_sem.at[1]
    )
    own_w.start()
    here = pl.ds(pl.multiple_of(sp * tokens, tokens), tokens)
    mine = pl.ds(pl.multiple_of(sp * hd, hd), hd)
    own_k = pltpu.make_async_copy(keys.at[0, :, mine], kraw.at[here], own_sem.at[2])
    own_v = pltpu.make_async_copy(values.at[0, :, mine], vb.at[here], own_sem.at[3])
    own_k.start()
    own_v.start()
    for p in range(3):
        kv_copy(0, p).start()
        kv_copy(1, p).start()

    def norm_rows(source, c):
        step = 32
        gain = mix_gain[...].reshape(1, width)

        def inner(i, carry):
            at = pl.multiple_of(c * part + i * step, step)
            wide = xraw[source, pl.ds(at, step), :].astype(jnp.float32)
            scale = lax.rsqrt(jnp.mean(wide * wide, axis=-1, keepdims=True) + norm_eps)
            done = (wide * scale * gain).astype(jnp.bfloat16)
            to = pl.ds(pl.multiple_of(source * tokens + at, step), step)
            for d in range(dp_count):
                xs[d, to, :] = done[:, d * depth : (d + 1) * depth]
            return carry

        lax.fori_loop(0, part // step, inner, 0)

    def accumulate(block, first=False):
        tile = 256
        for n in range(0, heads * hd, tile):
            term = jnp.dot(xs[block], wb[block, :, n : n + tile], preferred_element_type=jnp.float32)
            if first:
                acc[:, n : n + tile] = term
            else:
                acc[:, n : n + tile] += term

    own_x.wait()
    for c in range(chunks):
        norm_rows(sp, c)

    def pair_rows():
        for c in range(chunks):
            x_copy(pair, c, 1, pair).wait_recv()
            norm_rows(pair, c)

    def across_in(c):
        x_copy(across, c, 0, across).wait_recv()
        x_copy(across, c, 2, pair).start()

    def key_rows():
        own_k.wait()
        own_v.wait()
        for p in range(3):
            rows = pl.ds(pl.multiple_of(peers[p] * tokens, tokens), tokens)
            for buf, rsem, ssem in ((kraw, krecv, ksend), (vb, vrecv, vsend)):
                pltpu.make_async_remote_copy(
                    src_ref=buf.at[rows], dst_ref=buf.at[rows], send_sem=ssem.at[p],
                    recv_sem=rsem.at[peers[p]], device_id={"sp": peers[p]}, device_id_type=MESH,
                ).wait_recv()
        kn[...] = rms_scaled(kraw[...], key_gain[...].reshape(1, hd))

    steps = []
    for k in range(1, nz):
        for h in range(heads):
            steps.append((2 * k + h, -k, functools.partial(z_step, k, h)))
            steps.append((2 * k + h, -k, functools.partial(side_send, k, h, start)))
    steps.append((heads - 1, 0, functools.partial(both_send, 0, heads - 1)))
    for h in range(1, heads, 2):
        steps.append((2 * nz - 4 + h + 0.5, -nz, functools.partial(far_in_step, h)))
        steps.append((2 * nz - 1 + h, -nz, functools.partial(far_out_step, h)))
    steps.sort(key=lambda step: step[:2])

    def advance(limit):
        while steps and steps[0][0] <= limit:
            steps.pop(0)[2]()

    advance(3)
    pair_rows()
    advance(4)
    across_in(0)
    advance(6)
    norm_rows(across, 0)
    advance(7)
    across_in(1)
    norm_rows(across, 1)
    x_copy(corner, 0, 2, pair).wait_recv()
    norm_rows(corner, 0)
    advance(8)
    x_copy(corner, 1, 2, pair).wait_recv()
    norm_rows(corner, 1)
    own_w.wait()
    accumulate(dp, True)
    for h in range(heads):
        side_wait(0, h)
    accumulate(side)
    accumulate(order(1) * nx + x)
    key_rows()

    size = math.gcd(seq, row_block)
    rowi = lax.broadcasted_iota(jnp.int32, (size, size), 0)
    coli = lax.broadcasted_iota(jnp.int32, (size, size), 1)
    causal = coli < rowi
    suffix = (rowi >= coli).astype(jnp.float32).astype(jnp.bfloat16)

    def o_copy(h, p, incoming=False):
        peer = peers[p]
        owner = peer if incoming else sp
        return pltpu.make_async_remote_copy(
            src_ref=ob.at[h, pl.ds(pl.multiple_of(peer * tokens, tokens), tokens)],
            dst_ref=out.at[0, :, pl.ds(pl.multiple_of(owner * (heads * hd) + h * hd, hd), hd)],
            send_sem=osend.at[p, h], recv_sem=orecv.at[owner, h],
            device_id={"sp": peer}, device_id_type=MESH,
        )

    def o_local(h):
        return pltpu.make_async_copy(
            ob.at[h, here],
            out.at[0, :, pl.ds(pl.multiple_of(base + h * hd, hd), hd)],
            own_sem.at[4 + h],
        )

    for h in range(heads):
        advance(2 * nz + h if h else 2 * nz)
        cols = slice(h * hd, (h + 1) * hd)
        total = acc[:, cols]
        blocks = [order(rank) * nx + x for rank in range(2, nz)]
        for rank in range(1, nz):
            side_wait(rank, h)
            blocks.append(order(rank) * nx + (1 - x))
        for block in blocks:
            total = total + jnp.dot(
                xs[block], wb[block, :, cols], preferred_element_type=jnp.float32
            )
        qn = rms_scaled(total.astype(jnp.bfloat16), query_gain[...].reshape(1, hd))
        off = offset[sp * heads + h]
        for rb in range(seq // size):
            q = qn[rb * size : (rb + 1) * size]
            carry, result = None, None
            for kb in reversed(range(rb + 1)):
                at = slice(kb * size, (kb + 1) * size)
                s = lax.dot_general(
                    q, kn[at], (((1,), (1,)), ((), ())), preferred_element_type=jnp.float32
                )
                s = s * hd ** (-0.5) + off
                soft = jnp.log(1.0 + jnp.exp(s))
                if kb == rb:
                    soft = jnp.where(causal, soft, 0.0)
                upper = soft.astype(jnp.bfloat16)
                lower = (soft - upper.astype(jnp.float32)).astype(jnp.bfloat16)
                sums = jnp.dot(upper, suffix, preferred_element_type=jnp.float32) + jnp.dot(
                    lower, suffix, preferred_element_type=jnp.float32
                )
                if carry is not None:
                    sums = sums + carry
                carry = sums[:, 0:1]
                w = jnp.exp(s - sums)
                if kb == rb:
                    w = jnp.where(causal, w, 0.0)
                term = jnp.dot(w.astype(jnp.bfloat16), vb[at], preferred_element_type=jnp.float32)
                result = term if result is None else result + term
            ob[h, rb * size : (rb + 1) * size, :] = result.astype(jnp.bfloat16)
        for p in (0, 2, 1):
            o_copy(h, p).start()
        o_local(h).start()

    for h in range(heads):
        for k in range(nz):
            z_send(k, h, finish_send)
            side_send(k, h, finish_send)
        if h % 2:
            far_in(h, finish_send)
            far_out(h, finish_send)
    for c in range(chunks):
        x_copy(sp, c, 0, across).wait_send()
        x_copy(sp, c, 1, pair).wait_send()
        x_copy(across, c, 2, pair).wait_send()
    for p in range(3):
        kv_copy(0, p).wait_send()
        kv_copy(1, p).wait_send()
    for h in range(heads):
        o_local(h).wait()
        for p in range(3):
            o_copy(h, p).wait_send()
            o_copy(h, p, True).wait_recv()


def fused_body(nx, stream, mix_gain, query_weight, query_gain, keys, key_gain, values, stick_offset):
    sp_count = lax.axis_size("sp")
    dp_count = lax.axis_size("dp")
    nz = dp_count // nx
    tokens, width = stream.shape[1:]
    depth, columns = query_weight.shape
    hd = query_gain.shape[0]
    heads = stick_offset.shape[0] // sp_count
    seq = tokens * sp_count
    chunks = 2
    vmem = pl.BlockSpec(memory_space=pltpu.VMEM)
    hbm = pl.BlockSpec(memory_space=pl.ANY)
    dma = pltpu.SemaphoreType.DMA
    return pl.pallas_call(
        functools.partial(kernel, nz, nx, heads),
        out_shape=jax.ShapeDtypeStruct((1, tokens, columns), jnp.bfloat16),
        in_specs=[hbm, vmem, hbm, vmem, hbm, vmem, hbm, pl.BlockSpec(memory_space=pltpu.SMEM)],
        out_specs=hbm,
        scratch_shapes=[
            pltpu.VMEM((sp_count, tokens, width), jnp.bfloat16),
            pltpu.VMEM((dp_count, seq, depth), jnp.bfloat16),
            pltpu.VMEM((dp_count, depth, heads * hd), jnp.bfloat16),
            pltpu.VMEM((seq, hd), jnp.bfloat16),
            pltpu.VMEM((seq, hd), jnp.bfloat16),
            pltpu.VMEM((seq, hd), jnp.bfloat16),
            pltpu.VMEM((seq, heads * hd), jnp.float32),
            pltpu.VMEM((heads, seq, hd), jnp.bfloat16),
            dma((4 + heads,)),
            dma((dp_count, heads)),
            dma((2, nz, heads)),
            dma((nz, heads)),
            dma((2, heads)),
            dma((sp_count, chunks)),
            dma((3, chunks)),
            dma((sp_count,)),
            dma((3,)),
            dma((sp_count,)),
            dma((3,)),
            dma((sp_count, heads)),
            dma((3, heads)),
        ],
        compiler_params=pltpu.CompilerParams(
            collective_id=0, has_side_effects=True, vmem_limit_bytes=62 * 1024 * 1024
        ),
    )(
        stream, mix_gain, query_weight, query_gain, keys, key_gain, values,
        stick_offset,
    )


def widths(mesh):
    names = tuple(mesh.axis_names)
    grid = mesh.devices if names == ("dp", "sp") else mesh.devices.T
    nx = len({d.coords[0] for d in grid[:, 0]})
    ny = len({d.coords[1] for d in grid[0]})
    return nx, ny


def solution(mesh):
    nx, ny = widths(mesh)
    pairs = nx == 2 and ny == 2

    def body(*args):
        stream, _, _, query_gain, keys = args[:5]
        sp_count = lax.axis_size("sp")
        one_head = keys.shape[2] // query_gain.shape[0] == sp_count
        nz = lax.axis_size("dp") // nx
        if pairs and one_head and sp_count == 2 * ny and nz >= 4 and nz % 2 == 0:
            return fused_body(nx, *args)
        return general_body(*args)

    return jax.shard_map(
        body,
        mesh=mesh,
        in_specs=(
            P("dp", "sp", None),
            P(),
            P("dp", None),
            P(),
            P("dp", "sp", None),
            P(),
            P("dp", "sp", None),
            P(),
        ),
        out_specs=P("dp", "sp", None),
        check_vma=False,
    )
```
